32 devices in a mesh: dp: 4 (over y, x), kv: 4 (over z), tp: 2 (over core).
Axes of the slice: x: 2, y: 2, z: 4, core: 2. Of those that a mesh axis runs over, the one named last changes fastest.
Arguments:
- tokens: bfloat16 [4, 1024, 2048], P('dp', 'kv'), may hold values from -28 to 28, as said below
- query_weight: bfloat16 [2048, 768], P(None, 'tp'), may hold values from -0.125 to 0.125
- key_weight: bfloat16 [2048, 256], P(None, 'tp'), may hold values from -0.125 to 0.125
- value_weight: bfloat16 [2048, 256], P(None, 'tp'), may hold values from -0.125 to 0.125
- gate_weight: bfloat16 [2048, 24], replicated, may hold values from -0.125 to 0.125
- compress_weight: float32 [2, 32, 64], replicated, may hold values from -1 to 1
- out_weight: bfloat16 [768, 2048], P('tp'), may hold values from -0.21875 to 0.21875
- out_gain: float32 [2048], replicated, may hold values from 0.1 to 1.9
- chosen: int32 [4, 32, 16], P('dp', 'kv'), may hold values from -1 to 31, as said below
Outputs:
- output: float32 [4, 1024, 2048], P('dp', ('kv', 'tp'))
The draws below stay inside these ranges and needn't reach their ends.
Inputs may be any that keep to these rules, and one draw needn't show every extreme that they name: `chosen`: row q of a sequence lists distinct blocks; its first entry is q itself; the others are -1 or blocks held by an earlier index of kv (block index // 8). Over the rows of one kv index, at most 2 distinct blocks come from any other single index, and every index past the first reads exactly 2 blocks of the first index, among them block 0. `tokens`: finite activations; some rows are much larger than others in some draws.
All inputs are finite; a program needn't handle non-finite values.
Results may differ from the reference program's by a relative error of at most 0.02.
The reference program's roundings to bfloat16 on the way count: a program that leaves them out, or rounds other values in their place, can miss the bound.
Values may be sent and summed in bfloat16 or wider, within the bound.
A program may use at most 64 MiB of HBM per device.

```python
import jax
import jax.numpy as jnp
from jax import lax

D = 2048
KV_HEADS = 4
GROUP = 3
HEAD = 64
BLK = 32
TOPN = 16
CAP = 2
TOK_DEV = 256
HEADS = 12
SEQ = 1024
B = 4
KEY_BLOCKS = 32


def draw_tokens(key, part):
    base_key, scale_key = jax.random.split(key)
    return jnp.clip(jax.random.normal(base_key, (B, SEQ, D), jnp.float32), -6.0, 6.0).astype(jnp.bfloat16)


def draw_chosen(key, part):
    devices = SEQ // TOK_DEV
    blocks = TOK_DEV // BLK
    remote = blocks * (TOPN - 1)
    items = devices * CAP
    favour_key, pick_key, local_key, order_key = jax.random.split(key, 4)
    owner = jnp.arange(devices, dtype=jnp.int32)[None, None, :, None]
    device = jnp.arange(devices, dtype=jnp.int32)[None, :, None, None]
    copies = jnp.arange(CAP, dtype=jnp.int32)[None, None, None, :]
    shape = (B, devices, devices, CAP)
    favour = jax.random.randint(favour_key, (B, 1, devices, 1), 0, 4)
    taken = jax.random.randint(pick_key, shape, 0, 4) < favour
    forced = (owner == 0) | (copies == 0) & ((owner == device - 1) | (owner == device - devices // 2))
    level = jnp.where(owner < device, jnp.where(forced, 2, taken.astype(jnp.int32)), -1)
    item_index = owner * CAP + copies
    ranking = level * (items * items) + jax.random.randint(order_key, shape, 0, items) * items + item_index
    upper = jnp.broadcast_to((blocks - copies + CAP - 1) // CAP, shape)
    local_block = copies + CAP * jax.random.randint(local_key, shape, 0, upper)
    local_block = jnp.where((owner == 0) & (copies == 0), 0, local_block)
    global_id = jnp.where(level >= 1, owner * blocks + local_block, -1).reshape(B, devices, items)
    order = jnp.argsort(-ranking.reshape(B, devices, items), axis=-1)
    ranked = jnp.take_along_axis(global_id, order, axis=-1)
    if items >= remote:
        ranked = ranked[..., :remote]
    else:
        ranked = jnp.concatenate([ranked, jnp.full((B, devices, remote - items), -1, jnp.int32)], axis=-1)
    remote_part = jnp.swapaxes(ranked.reshape(B, devices, TOPN - 1, blocks), 2, 3)
    diagonal = jnp.arange(devices, dtype=jnp.int32)[:, None] * blocks + jnp.arange(blocks, dtype=jnp.int32)[None, :]
    diagonal = jnp.broadcast_to(diagonal[None, :, :, None], (B, devices, blocks, 1))
    listed = jnp.concatenate([diagonal, remote_part.astype(jnp.int32)], axis=-1)
    return listed.reshape(B, devices * blocks, TOPN).astype(jnp.int32)


def steps_of(rng, shape, shards, smallest, high):
    factor_of, own = 1.0, jax.random.fold_in(rng, 6)
    for axis_at, blocks in shards:
        draws = jnp.exp(jax.random.uniform(jax.random.fold_in(own, axis_at), (blocks,), jnp.float32, smallest / len(shards), high / len(shards)))
        factor_of = factor_of * jnp.repeat(draws, shape[axis_at] // blocks).reshape([-1 if axis == axis_at else 1 for axis in range(len(shape))])
    return factor_of


def noise(key, extent, deviation, reach, pieces=(), held_as=jnp.bfloat16):
    level = steps_of(key, extent, pieces, -0.22, 0.18) if pieces else 1.0
    drawn = jax.random.normal(key, extent, jnp.float32) * deviation * level
    return jnp.minimum(jnp.maximum(drawn, -reach), reach).astype(held_as)


def setup_inputs(seed: int = 0) -> dict:
    key_of = jax.random.split(jax.random.key(seed), 10)
    return {
        "tokens": draw_tokens(jax.random.fold_in(key_of[9], 71), 0),
        "query_weight": noise(key_of[1], (D, HEADS * HEAD), D ** -0.5, 0.125, ((1, 2),)),
        "key_weight": noise(key_of[2], (D, KV_HEADS * HEAD), D ** -0.5, 0.125, ((1, 2),)),
        "value_weight": noise(key_of[3], (D, KV_HEADS * HEAD), D ** -0.5, 0.125, ((1, 2),)),
        "gate_weight": noise(key_of[4], (D, 2 * HEADS), D ** -0.5, 0.125),
        "compress_weight": noise(key_of[5], (2, BLK, HEAD), BLK ** -0.5, 1.0, (), jnp.float32),
        "out_weight": noise(key_of[6], (HEADS * HEAD, D), (HEADS * HEAD) ** -0.5, 0.21875, ((0, 2),)),
        "out_gain": jnp.clip(1.0 + 0.18 * jax.random.normal(key_of[7], (D,), jnp.float32), 0.1, 1.9),
        "chosen": draw_chosen(jax.random.fold_in(key_of[9], 71), 0),
    }


neg_big = -1e+30
rope_base = 500000.0
norm_eps = 1e-06

def rotate(array_in, positions):
    half_dim = array_in.shape[-1] // 2
    inverse = rope_base ** (-jnp.arange(half_dim, dtype=jnp.float32) * (2.0 / array_in.shape[-1]))
    angles = positions.astype(jnp.float32)[:, None] * inverse[None, :]
    cosine = jnp.cos(angles)[:, None, :]
    sine_vals = jnp.sin(angles)[:, None, :]
    floats = array_in.astype(jnp.float32)
    first_half = floats[..., :half_dim]
    second_half = floats[..., half_dim:]
    turned = jnp.concatenate([first_half * cosine - second_half * sine_vals, second_half * cosine + first_half * sine_vals], axis=-1)
    return turned.astype(jnp.bfloat16)

def reference(tokens, query_weight, key_weight, value_weight, gate_weight, compress_weight, out_weight, out_gain, chosen):
    flattened = tokens.reshape(B * SEQ, D)
    queries = jnp.dot(flattened, query_weight, preferred_element_type=jnp.float32).astype(jnp.bfloat16)
    key_rows = jnp.dot(flattened, key_weight, preferred_element_type=jnp.float32).astype(jnp.bfloat16).reshape(B, SEQ, KV_HEADS, HEAD)
    values = jnp.dot(flattened, value_weight, preferred_element_type=jnp.float32).astype(jnp.bfloat16).reshape(B, SEQ, KV_HEADS, HEAD)
    gate_values = jax.nn.sigmoid(jnp.dot(flattened, gate_weight, preferred_element_type=jnp.float32)).reshape(B, SEQ, 2, KV_HEADS, GROUP)
    positions = jnp.arange(SEQ, dtype=jnp.int32)
    plain_query = queries.reshape(B, SEQ, KV_HEADS, GROUP, HEAD)
    turned_query = rotate(queries.reshape(B, SEQ, HEADS, HEAD), positions).reshape(B, SEQ, KV_HEADS, GROUP, HEAD)
    turned_keys = rotate(key_rows, positions)
    key_blocks = key_rows.reshape(B, KEY_BLOCKS, BLK, KV_HEADS, HEAD).astype(jnp.float32)
    val_blocks = values.reshape(B, KEY_BLOCKS, BLK, KV_HEADS, HEAD).astype(jnp.float32)
    packed_keys = jnp.einsum('bnjhd,jd->bnhd', key_blocks, compress_weight[0], precision=lax.Precision.HIGHEST).astype(jnp.bfloat16).astype(jnp.float32)
    packed_values = jnp.einsum('bnjhd,jd->bnhd', val_blocks, compress_weight[1], precision=lax.Precision.HIGHEST).astype(jnp.bfloat16).astype(jnp.float32)
    turned_blocks = turned_keys.reshape(B, KEY_BLOCKS, BLK, KV_HEADS, HEAD)
    value_blocks = values.reshape(B, KEY_BLOCKS, BLK, KV_HEADS, HEAD)
    score_scale = HEAD ** (-0.5)
    batch_index = jnp.arange(B, dtype=jnp.int32)[:, None]

    def one_block(block_index):
        first_row = block_index * BLK
        plain_block = lax.dynamic_slice_in_dim(plain_query, first_row, BLK, 1).astype(jnp.float32)
        turned_block = lax.dynamic_slice_in_dim(turned_query, first_row, BLK, 1).astype(jnp.float32)
        block_pos = first_row + jnp.arange(BLK, dtype=jnp.int32)
        scores = jnp.einsum('bqhgd,bnhd->bqhgn', plain_block, packed_keys) * score_scale
        visible = ((jnp.arange(KEY_BLOCKS, dtype=jnp.int32) + 1) * BLK - 1)[None, :] <= block_pos[:, None]
        keep_mask = visible[None, :, None, None, :]
        scores = jnp.where(keep_mask, scores, neg_big)
        peak = lax.optimization_barrier(jnp.max(scores, axis=-1, keepdims=True))
        powers = jnp.where(keep_mask, jnp.exp(scores - peak), 0.0)
        weight = (powers / jnp.maximum(lax.optimization_barrier(jnp.sum(powers, axis=-1, keepdims=True)), 1.0)).astype(jnp.bfloat16)
        weight = lax.optimization_barrier(weight).astype(jnp.float32)
        coarse_out = jnp.einsum('bqhgn,bnhd->bqhgd', weight, packed_values)
        picked = chosen[:, block_index]
        usable = picked >= 0
        clipped = jnp.maximum(picked, 0)
        sel_keys = turned_blocks[batch_index, clipped].astype(jnp.float32)
        sel_values = value_blocks[batch_index, clipped].astype(jnp.float32)
        key_pos = clipped[:, :, None] * BLK + jnp.arange(BLK, dtype=jnp.int32)[None, None, :]
        allowed = usable[:, None, :, None] & (key_pos[:, None, :, :] <= block_pos[None, :, None, None])
        fine_mask = allowed[:, :, None, None, :, :]
        fine = jnp.einsum('bqhgd,btjhd->bqhgtj', turned_block, sel_keys) * score_scale
        fine = jnp.where(fine_mask, fine, neg_big)
        fine_peak = lax.optimization_barrier(jnp.max(fine, axis=(-2, -1), keepdims=True))
        fine_powers = jnp.where(fine_mask, jnp.exp(fine - fine_peak), 0.0)
        fine_total = lax.optimization_barrier(jnp.sum(fine_powers, axis=(-2, -1)))
        rounded = lax.optimization_barrier(fine_powers.astype(jnp.bfloat16)).astype(jnp.float32)
        fine_out = jnp.einsum('bqhgtj,btjhd->bqhgd', rounded, sel_values) / fine_total[..., None]
        gate_block = lax.dynamic_slice_in_dim(gate_values, first_row, BLK, 1)
        mixed = gate_block[:, :, 0][..., None] * coarse_out + gate_block[:, :, 1][..., None] * fine_out
        return mixed.astype(jnp.bfloat16).reshape(B, BLK, HEADS * HEAD)
    hidden = lax.map(one_block, jnp.arange(KEY_BLOCKS, dtype=jnp.int32))
    hidden = jnp.moveaxis(hidden, 0, 1).reshape(B * SEQ, HEADS * HEAD)
    summed = jnp.dot(hidden, out_weight, preferred_element_type=jnp.float32)
    normed = summed * lax.rsqrt(lax.optimization_barrier(jnp.mean(summed * summed, axis=-1, keepdims=True)) + norm_eps) * out_gain
    return normed.astype(jnp.float32).reshape(B, SEQ, D)
```

```python
import functools

import numpy as np
import jax
import jax.numpy as jnp
from jax import lax
from jax.experimental import pallas as pl
from jax.experimental.pallas import tpu as pltpu
from jax.sharding import PartitionSpec as P

HEAD = 64
BLK = 32
CAP = 2
NEG = -1e30
ROPE_BASE = 500000.0
EPS = 1e-06
F32 = jnp.float32
BF = jnp.bfloat16
ANY = pl.BlockSpec(memory_space=pl.ANY)


def mm(a, b):
    return jnp.dot(a, b, preferred_element_type=F32)


def mm_t(a, b):
    return lax.dot_general(a, b, (((1,), (1,)), ((), ())), preferred_element_type=F32)


def iota(shape, dim):
    return lax.broadcasted_iota(jnp.int32, shape, dim)


def rope_table(kvn, length):
    half = HEAD // 2
    inverse = ROPE_BASE ** (-np.arange(half) * (2.0 / HEAD))
    angles = np.arange(kvn * length)[None, :] * inverse[:, None]
    table = np.stack([np.cos(angles), np.sin(angles)]).astype(np.float32)
    return table.reshape(2, half, kvn, length).transpose(2, 0, 1, 3).copy()


def kernel(
    kvn,
    tpn,
    tok_h,
    wq_h,
    wk_h,
    wv_h,
    wg_h,
    cw_h,
    wo_h,
    gain_h,
    chosen_h,
    tab_h,
    out_h,
    tok,
    wkv,
    wq,
    wg,
    cw,
    wo,
    wo2,
    gain,
    chosen,
    tab,
    reqs,
    reqin,
    maskb,
    tkv,
    vt,
    coarse,
    blk_out,
    blks,
    qp,
    qt,
    gt,
    mixt,
    mix_own,
    mix_out,
    mix_in,
    acc,
    lsem,
    osem,
    req_s,
    req_r,
    co_s,
    co_r,
    bl_s,
    bl_r,
    wo_s,
    wo_r,
    mx_s,
    mx_r,
):
    dp = lax.axis_index("dp")
    me = lax.axis_index("kv")
    tp = lax.axis_index("tp")
    length, width = tok.shape
    cols = wkv.shape[1] // 2
    kv_dev = cols // HEAD
    heads = wq.shape[1] // HEAD
    per_kv = heads // kv_dev
    nb = length // BLK
    total_blocks = kvn * nb
    rows_out = length // tpn
    slot_rows = CAP * BLK

    def local(src, dst, index):
        return pltpu.make_async_copy(src, dst, lsem.at[index])

    loads = [
        local(chosen_h.at[0], chosen, 0),
        local(tab_h.at[me], tab, 1),
        local(tok_h.at[0], tok, 2),
        local(wk_h, wkv.at[:, 0:cols], 3),
        local(wv_h, wkv.at[:, cols : 2 * cols], 4),
        local(cw_h, cw, 5),
        local(wq_h, wq, 6),
        local(wg_h, wg, 7),
        local(wo_h, wo, 8),
        local(gain_h, gain, 9),
    ]
    for load in loads:
        load.start()

    barrier = pltpu.get_barrier_semaphore()
    for d in range(1, kvn):
        peer = lax.rem(me + d, kvn)
        pl.semaphore_signal(
            barrier, inc=1, device_id=(dp, peer, tp), device_id_type=pl.DeviceIdType.MESH
        )
    other = (dp, me, tpn - 1 - tp)
    pl.semaphore_signal(barrier, inc=1, device_id=other, device_id_type=pl.DeviceIdType.MESH)

    def remote(src, dst, send, recv, target):
        return pltpu.make_async_remote_copy(
            src_ref=src,
            dst_ref=dst,
            send_sem=send,
            recv_sem=recv,
            device_id=target,
            device_id_type=pl.DeviceIdType.MESH,
        )

    def req_copy(d):
        return remote(
            reqs.at[d], reqin.at[d], req_s.at[d], req_r.at[d], (dp, lax.rem(me - d + kvn, kvn), tp)
        )

    def coarse_copy(d):
        return remote(
            coarse.at[0], coarse.at[d], co_s.at[d], co_r.at[d], (dp, lax.rem(me + d, kvn), tp)
        )

    def block_copy(d):
        return remote(
            blk_out.at[d - 1],
            blks.at[d - 1],
            bl_s.at[d],
            bl_r.at[d],
            (dp, lax.rem(me + d, kvn), tp),
        )

    weight_copy = remote(wo_h, wo2, wo_s, wo_r, other)
    mix_copy = remote(mix_out, mix_in, mx_s, mx_r, other)

    for d in range(1, kvn):

        @pl.when(me < d)
        def _():
            blks[d - 1] = jnp.zeros(blks.shape[1:], BF)
            coarse[d] = jnp.zeros(coarse.shape[1:], F32)

    loads[0].wait()
    listed = chosen[...]
    lane_blk = iota((nb, total_blocks), 1)
    hit = jnp.zeros((nb, total_blocks), F32)
    for t in range(listed.shape[1]):
        hit = jnp.where(listed[:, t : t + 1] == lane_blk, 1.0, hit)
    needed = jnp.max(hit, axis=0, keepdims=True)
    gi = iota((total_blocks, total_blocks), 0)
    gj = iota((total_blocks, total_blocks), 1)
    before = jnp.where((gi // nb == gj // nb) & (gi < gj), 1.0, 0.0).astype(BF)
    rank = mm(jnp.broadcast_to(needed, (8, total_blocks)).astype(BF), before)[0:1]
    ra = iota((kvn * 8, total_blocks), 0)
    ja = iota((kvn * 8, total_blocks), 1)
    pick = jnp.where(
        (needed > 0.5)
        & (rank == (ra % 8).astype(F32))
        & (ra % 8 < CAP)
        & (ja // nb == me - ra // 8),
        1.0,
        0.0,
    )
    wanted = jnp.sum(pick * ((ja % nb) + 1).astype(F32), axis=1, keepdims=True) - 1.0
    reqs[...] = jnp.broadcast_to(wanted, (kvn * 8, 128)).reshape(kvn, 8, 128)

    pl.semaphore_wait(barrier, kvn)
    for d in range(1, kvn):

        @pl.when(me >= d)
        def _():
            req_copy(d).start()

    weight_copy.start()
    spread = jnp.where(iota((nb, length), 1) // BLK == iota((nb, length), 0), 1.0, 0.0)
    member = mm(mm_t(pick, hit), spread)
    maskb[...] = jnp.where(member > 0.5, 0.0, NEG)

    loads[1].wait()
    cos_t = tab[0]
    sin_t = tab[1]
    cos_n = jnp.concatenate([cos_t, cos_t] * kv_dev, axis=0).T
    sin_n = jnp.concatenate([-sin_t, sin_t] * kv_dev, axis=0).T

    for index in (2, 3, 4, 5):
        loads[index].wait()
    both = mm(tok[...], wkv[...]).astype(BF)
    tkv[:, cols : 2 * cols] = both[:, cols : 2 * cols]
    both = both.astype(F32)
    key_f = both[:, 0:cols]
    val_f = both[:, cols : 2 * cols]

    def compress(x, index):
        weight = jnp.concatenate([cw[index]] * kv_dev, axis=1)
        packed = jnp.sum(x.reshape(nb, BLK, cols) * weight[None], axis=1)
        return packed.astype(BF).astype(F32)

    coarse[0, 0:nb] = compress(key_f, 0)
    coarse[0, nb : 2 * nb] = compress(val_f, 1)
    for d in range(1, kvn):

        @pl.when(me + d < kvn)
        def _():
            coarse_copy(d).start()

    half = HEAD // 2
    low = iota((length, cols), 1) % HEAD < half
    swapped = jnp.where(low, pltpu.roll(key_f, cols - half, 1), pltpu.roll(key_f, half, 1))
    tkv[:, 0:cols] = (key_f * cos_n + swapped * sin_n).astype(BF)

    si = iota((slot_rows, length), 0)
    sj = iota((slot_rows, length), 1)
    for d in range(1, kvn):

        @pl.when(me + d < kvn)
        def _():
            req_copy(d).wait_recv()
            tile = reqin[d]
            ask = jnp.concatenate(
                [jnp.broadcast_to(tile[s : s + 1], (BLK, 128)) for s in range(CAP)], axis=0
            )
            ask = jnp.concatenate([ask] * (length // 128), axis=1)
            chooser = jnp.where(
                (ask == (sj // BLK).astype(F32)) & (si % BLK == sj % BLK), 1.0, 0.0
            ).astype(BF)
            sent = mm(chooser, tkv[...]).astype(BF)
            blk_out[d - 1, 0:slot_rows] = sent[:, 0:cols]
            blk_out[d - 1, slot_rows : 2 * slot_rows] = sent[:, cols : 2 * cols]
            block_copy(d).start()

    vt[...] = val_f.T.astype(BF)

    loads[6].wait()
    scale = HEAD ** (-0.5)
    query_t = mm(tok[...], wq[...]).astype(BF).astype(F32).T * scale
    qp[...] = query_t.astype(BF)
    for h in range(heads):
        first = query_t[h * HEAD : h * HEAD + half]
        second = query_t[h * HEAD + half : (h + 1) * HEAD]
        qt[h * HEAD : h * HEAD + half] = (first * cos_t - second * sin_t).astype(BF)
        qt[h * HEAD + half : (h + 1) * HEAD] = (second * cos_t + first * sin_t).astype(BF)
    loads[7].wait()
    gates = jax.nn.sigmoid(mm_t(wg[...], tok[...]))
    for branch in range(2):
        mine = jnp.zeros((heads, length), F32)
        for t in range(tpn):
            row = (branch * tpn + t) * heads
            mine = jnp.where(tp == t, gates[row : row + heads], mine)
        gt[branch * heads : (branch + 1) * heads] = mine

    for d in range(1, kvn):

        @pl.when(me >= d)
        def _():
            coarse_copy(d).wait_recv()

    coarse_k = coarse[:, 0:nb].reshape(kvn * nb, cols)
    coarse_vt = coarse[:, nb : 2 * nb].reshape(kvn * nb, cols).T
    ck = [coarse_k[:, k * HEAD : (k + 1) * HEAD].astype(BF) for k in range(kv_dev)]
    cvt = [coarse_vt[k * HEAD : (k + 1) * HEAD].astype(BF) for k in range(kv_dev)]

    for d in range(1, kvn):

        @pl.when(me >= d)
        def _():
            block_copy(d).wait_recv()

    far = (kvn - 1) * slot_rows
    far_k = blks[:, 0:slot_rows].reshape(far, cols)
    far_vt = blks[:, slot_rows : 2 * slot_rows].reshape(far, cols).astype(F32).T.astype(BF)
    kr = [far_k[:, k * HEAD : (k + 1) * HEAD] for k in range(kv_dev)]
    vr = [far_vt[k * HEAD : (k + 1) * HEAD] for k in range(kv_dev)]

    n = rows_out
    dk = iota((n, n), 0)
    dq = iota((n, n), 1)
    near_bias = jnp.where((dk // BLK == dq // BLK) & (dk <= dq), 0.0, NEG)
    cr = iota((kvn * nb, n), 0)
    cb = (me - cr // nb) * nb + cr % nb

    def attend(chunk):
        start = pl.multiple_of(chunk * n, n)
        here = pl.ds(start, n)
        far_bias = jnp.concatenate(
            [
                jnp.broadcast_to(maskb[d * 8 + s : d * 8 + s + 1, here], (BLK, n))
                for d in range(1, kvn)
                for s in range(CAP)
            ],
            axis=0,
        )
        pos = me * length + start + iota((kvn * nb, n), 1)
        seen = (cb >= 0) & ((cb + 1) * BLK - 1 <= pos)
        near_k = tkv[here, 0:cols]
        kd = [near_k[:, k * HEAD : (k + 1) * HEAD] for k in range(kv_dev)]
        for h in range(heads):
            k = h // per_kv
            rows = slice(h * HEAD, (h + 1) * HEAD)
            sc = jnp.where(seen, mm(ck[k], qp[rows, here]), NEG)
            peak = jnp.max(sc, axis=0, keepdims=True)
            pw = jnp.where(seen, jnp.exp(sc - peak), 0.0)
            weight = pw / jnp.maximum(jnp.sum(pw, axis=0, keepdims=True), 1.0)
            coarse_out = mm(cvt[k], weight.astype(BF))
            query = qt[rows, here]
            sf = mm(kr[k], query) + far_bias
            sn = mm(kd[k], query) + near_bias
            top = jnp.maximum(
                jnp.max(sf, axis=0, keepdims=True), jnp.max(sn, axis=0, keepdims=True)
            )
            pf = jnp.exp(sf - top)
            pn = jnp.exp(sn - top)
            norm = jnp.sum(pf, axis=0, keepdims=True) + jnp.sum(pn, axis=0, keepdims=True)
            fine = mm(vr[k], pf.astype(BF)) + mm(
                vt[k * HEAD : (k + 1) * HEAD, here], pn.astype(BF)
            )
            g_coarse = gt[h : h + 1, here]
            g_fine = gt[heads + h : heads + h + 1, here]
            mixt[rows] = g_coarse * coarse_out + fine * (g_fine / norm)
        return mixt[...].T.astype(BF)

    mix_out[...] = attend(tpn - 1 - tp)
    mix_copy.start()
    mix_own[...] = attend(tp)
    loads[8].wait()
    step = 512
    for c in range(0, width, step):
        acc[:, c : c + step] = mm(mix_own[...], wo[:, c : c + step])
    loads[9].wait()
    weight_copy.wait_recv()
    mix_copy.wait_recv()
    square = jnp.zeros((n, 1), F32)
    for c in range(0, width, step):
        part = acc[:, c : c + step] + mm(mix_in[...], wo2[:, c : c + step])
        acc[:, c : c + step] = part
        square = square + jnp.sum(part * part, axis=1, keepdims=True)
    factor = lax.rsqrt(square * (1.0 / width) + EPS)
    pieces = 4
    span = n // pieces
    stores = []
    for i in range(pieces):
        rows = slice(i * span, (i + 1) * span)
        acc[rows] = acc[rows] * factor[rows] * gain[...]
        store = pltpu.make_async_copy(acc.at[pl.ds(i * span, span)], out_h.at[0, pl.ds(i * span, span)], osem.at[i])
        store.start()
        stores.append(store)
    for store in stores:
        store.wait()
    weight_copy.wait_send()
    mix_copy.wait_send()
    for d in range(1, kvn):

        @pl.when(me >= d)
        def _():
            req_copy(d).wait_send()

        @pl.when(me + d < kvn)
        def _():
            coarse_copy(d).wait_send()
            block_copy(d).wait_send()


def on_device(kvn, tpn, tokens, wq, wk, wv, wg, cw, wo, gain, chosen):
    length, width = tokens.shape[1:]
    cols = wk.shape[1]
    qcols = wq.shape[1]
    table = jnp.asarray(rope_table(kvn, length))
    nb = length // BLK
    rows_out = length // tpn
    V = pltpu.VMEM
    dma = pltpu.SemaphoreType.DMA
    scratch = [
        V((length, width), BF),
        V((width, 2 * cols), BF),
        V((width, qcols), BF),
        V((wg.shape[1], width), BF),
        V(cw.shape, F32),
        V(wo.shape, BF),
        V(wo.shape, BF),
        V((1, width), F32),
        V(chosen.shape[1:], jnp.int32),
        V(table.shape[1:], F32),
        V((kvn, 8, 128), F32),
        V((kvn, 8, 128), F32),
        V((kvn * 8, length), F32),
        V((length, 2 * cols), BF),
        V((cols, length), BF),
        V((kvn, 2 * nb, cols), F32),
        V((kvn - 1, 2 * CAP * BLK, cols), BF),
        V((kvn - 1, 2 * CAP * BLK, cols), BF),
        V((qcols, length), BF),
        V((qcols, length), BF),
        V((wg.shape[1] // tpn, length), F32),
        V((qcols, rows_out), F32),
        V((rows_out, qcols), BF),
        V((rows_out, qcols), BF),
        V((rows_out, qcols), BF),
        V((rows_out, width), F32),
        dma((10,)),
        dma((4,)),
        dma((kvn,)),
        dma((kvn,)),
        dma((kvn,)),
        dma((kvn,)),
        dma((kvn,)),
        dma((kvn,)),
        dma,
        dma,
        dma,
        dma,
    ]
    return pl.pallas_call(
        functools.partial(kernel, kvn, tpn),
        out_shape=jax.ShapeDtypeStruct((1, rows_out, width), F32),
        in_specs=[ANY] * 10,
        out_specs=ANY,
        scratch_shapes=scratch,
        compiler_params=pltpu.CompilerParams(
            collective_id=0, has_side_effects=True, vmem_limit_bytes=67043328
        ),
    )(tokens, wq, wk, wv, wg.T, cw, wo, gain.reshape(1, width), chosen, table)


def solution(mesh):
    in_specs = (
        P("dp", "kv", None),
        P(None, "tp"),
        P(None, "tp"),
        P(None, "tp"),
        P(),
        P(),
        P("tp", None),
        P(),
        P("dp", "kv", None),
    )
    return jax.shard_map(
        functools.partial(on_device, mesh.shape["kv"], mesh.shape["tp"]),
        mesh=mesh,
        in_specs=in_specs,
        out_specs=P("dp", ("kv", "tp"), None),
        check_vma=False,
    )
```

```python
import functools

import numpy as np
import jax
import jax.numpy as jnp
from jax import lax
from jax.experimental import pallas as pl
from jax.experimental.pallas import tpu as pltpu
from jax.sharding import PartitionSpec as P

HEAD = 64
BLK = 32
CAP = 2
NEG = -1e30
ROPE_BASE = 500000.0
EPS = 1e-06
F32 = jnp.float32
BF = jnp.bfloat16
ANY = pl.BlockSpec(memory_space=pl.ANY)


def mm(a, b):
    return jnp.dot(a, b, preferred_element_type=F32)


def mm_t(a, b):
    return lax.dot_general(a, b, (((1,), (1,)), ((), ())), preferred_element_type=F32)


def iota(shape, dim):
    return lax.broadcasted_iota(jnp.int32, shape, dim)


def rope_table(kvn, length):
    half = HEAD // 2
    inverse = ROPE_BASE ** (-np.arange(half) * (2.0 / HEAD))
    angles = np.arange(kvn * length)[None, :] * inverse[:, None]
    table = np.stack([np.cos(angles), np.sin(angles)]).astype(np.float32)
    return table.reshape(2, half, kvn, length).transpose(2, 0, 1, 3).copy()


def kernel(
    kvn,
    tpn,
    tok_h,
    wq_h,
    wk_h,
    wv_h,
    wg_h,
    cw_h,
    wo_h,
    gain_h,
    chosen_h,
    tab_h,
    out_h,
    tok,
    wkv,
    wq,
    wg,
    cw,
    wo,
    wo2,
    gain,
    chosen,
    tab,
    reqs,
    reqin,
    maskb,
    tkv,
    vt,
    coarse,
    blk_out,
    blks,
    qp,
    qt,
    gt,
    part_c,
    part_n,
    part_m,
    part_l,
    mix_own,
    mix_out,
    mix_in,
    acc,
    lsem,
    osem,
    req_s,
    req_r,
    co_s,
    co_r,
    bl_s,
    bl_r,
    wo_s,
    wo_r,
    mx_s,
    mx_r,
):
    dp = lax.axis_index("dp")
    me = lax.axis_index("kv")
    tp = lax.axis_index("tp")
    length, width = tok.shape
    cols = wkv.shape[1] // 2
    kv_dev = cols // HEAD
    heads = wq.shape[1] // HEAD
    per_kv = heads // kv_dev
    nb = length // BLK
    total_blocks = kvn * nb
    rows_out = length // tpn
    slot_rows = CAP * BLK

    def local(src, dst, index):
        return pltpu.make_async_copy(src, dst, lsem.at[index])

    loads = [
        local(chosen_h.at[0], chosen, 0),
        local(tab_h.at[me], tab, 1),
        local(tok_h.at[0], tok, 2),
        local(wk_h, wkv.at[:, 0:cols], 3),
        local(wv_h, wkv.at[:, cols : 2 * cols], 4),
        local(cw_h, cw, 5),
        local(wq_h, wq, 6),
        local(wg_h, wg, 7),
        local(wo_h, wo, 8),
        local(gain_h, gain, 9),
    ]
    for load in loads:
        load.start()

    barrier = pltpu.get_barrier_semaphore()
    for d in range(1, kvn):
        peer = lax.rem(me + d, kvn)
        pl.semaphore_signal(
            barrier, inc=1, device_id=(dp, peer, tp), device_id_type=pl.DeviceIdType.MESH
        )
    other = (dp, me, tpn - 1 - tp)
    pl.semaphore_signal(barrier, inc=1, device_id=other, device_id_type=pl.DeviceIdType.MESH)

    def remote(src, dst, send, recv, target):
        return pltpu.make_async_remote_copy(
            src_ref=src,
            dst_ref=dst,
            send_sem=send,
            recv_sem=recv,
            device_id=target,
            device_id_type=pl.DeviceIdType.MESH,
        )

    def req_copy(d):
        return remote(
            reqs.at[d], reqin.at[d], req_s.at[d], req_r.at[d], (dp, lax.rem(me - d + kvn, kvn), tp)
        )

    def coarse_copy(d):
        return remote(
            coarse.at[0], coarse.at[d], co_s.at[d], co_r.at[d], (dp, lax.rem(me + d, kvn), tp)
        )

    def block_copy(d):
        return remote(
            blk_out.at[d - 1],
            blks.at[d - 1],
            bl_s.at[d],
            bl_r.at[d],
            (dp, lax.rem(me + d, kvn), tp),
        )

    weight_copy = remote(wo_h, wo2, wo_s, wo_r, other)
    mix_copy = remote(mix_out, mix_in, mx_s, mx_r, other)

    for d in range(1, kvn):

        @pl.when(me < d)
        def _():
            blks[d - 1] = jnp.zeros(blks.shape[1:], BF)
            coarse[d] = jnp.zeros(coarse.shape[1:], F32)

    loads[0].wait()
    listed = chosen[...]
    lane_blk = iota((nb, total_blocks), 1)
    hit = jnp.zeros((nb, total_blocks), F32)
    for t in range(listed.shape[1]):
        hit = jnp.where(listed[:, t : t + 1] == lane_blk, 1.0, hit)
    needed = jnp.max(hit, axis=0, keepdims=True)
    gi = iota((total_blocks, total_blocks), 0)
    gj = iota((total_blocks, total_blocks), 1)
    before = jnp.where((gi // nb == gj // nb) & (gi < gj), 1.0, 0.0).astype(BF)
    rank = mm(jnp.broadcast_to(needed, (8, total_blocks)).astype(BF), before)[0:1]
    ra = iota((kvn * 8, total_blocks), 0)
    ja = iota((kvn * 8, total_blocks), 1)
    pick = jnp.where(
        (needed > 0.5)
        & (rank == (ra % 8).astype(F32))
        & (ra % 8 < CAP)
        & (ja // nb == me - ra // 8),
        1.0,
        0.0,
    )
    wanted = jnp.sum(pick * ((ja % nb) + 1).astype(F32), axis=1, keepdims=True) - 1.0
    reqs[...] = jnp.broadcast_to(wanted, (kvn * 8, 128)).reshape(kvn, 8, 128)

    loads[1].wait()
    cos_t = tab[0]
    sin_t = tab[1]
    cos_n = jnp.concatenate([cos_t, cos_t] * kv_dev, axis=0).T
    sin_n = jnp.concatenate([-sin_t, sin_t] * kv_dev, axis=0).T

    for index in (2, 3, 4, 5):
        loads[index].wait()
    both = mm(tok[...], wkv[...]).astype(BF)
    tkv[:, cols : 2 * cols] = both[:, cols : 2 * cols]
    both = both.astype(F32)
    key_f = both[:, 0:cols]
    val_f = both[:, cols : 2 * cols]

    def compress(x, index):
        weight = jnp.concatenate([cw[index]] * kv_dev, axis=1)
        packed = jnp.sum(x.reshape(nb, BLK, cols) * weight[None], axis=1)
        return packed.astype(BF).astype(F32)

    coarse[0, 0:nb] = compress(key_f, 0)
    coarse[0, nb : 2 * nb] = compress(val_f, 1)
    half = HEAD // 2
    low = iota((length, cols), 1) % HEAD < half
    swapped = jnp.where(low, pltpu.roll(key_f, cols - half, 1), pltpu.roll(key_f, half, 1))
    tkv[:, 0:cols] = (key_f * cos_n + swapped * sin_n).astype(BF)

    vt[...] = val_f.T.astype(BF)

    pl.semaphore_wait(barrier, kvn)
    for d in range(1, kvn):

        @pl.when(me >= d)
        def _():
            req_copy(d).start()

    for d in range(1, kvn):

        @pl.when(me + d < kvn)
        def _():
            coarse_copy(d).start()

    weight_copy.start()
    spread = jnp.where(iota((nb, length), 1) // BLK == iota((nb, length), 0), 1.0, 0.0)
    member = mm(mm_t(pick, hit), spread)
    maskb[...] = jnp.where(member > 0.5, 0.0, NEG)


    loads[6].wait()
    n = rows_out
    scale = HEAD ** (-0.5)
    query_t = mm(tok[...], wq[...]).astype(BF).astype(F32).T * scale
    loads[7].wait()
    gates = jax.nn.sigmoid(mm_t(wg[...], tok[...]))
    for h in range(heads):
        k, g = h // per_kv, h % per_kv
        first = query_t[h * HEAD : h * HEAD + half]
        second = query_t[h * HEAD + half : (h + 1) * HEAD]
        plain = query_t[h * HEAD : (h + 1) * HEAD].astype(BF)
        turned_low = (first * cos_t - second * sin_t).astype(BF)
        turned_high = (second * cos_t + first * sin_t).astype(BF)
        for c in range(tpn):
            lanes = slice(g * n, (g + 1) * n)
            here = slice(c * n, (c + 1) * n)
            qp[c, k, :, lanes] = plain[:, here]
            qt[c, k, 0:half, lanes] = turned_low[:, here]
            qt[c, k, half:HEAD, lanes] = turned_high[:, here]
            for branch in range(2):
                gate = jnp.zeros((1, n), F32)
                for t in range(tpn):
                    row = (branch * tpn + t) * heads + h
                    gate = jnp.where(tp == t, gates[row : row + 1, here], gate)
                gt[c, branch * kv_dev + k : branch * kv_dev + k + 1, lanes] = gate

    si = iota((slot_rows, length), 0)
    sj = iota((slot_rows, length), 1)
    for d in range(1, kvn):

        @pl.when(me + d < kvn)
        def _():
            req_copy(d).wait_recv()
            tile = reqin[d]
            ask = jnp.concatenate(
                [jnp.broadcast_to(tile[s : s + 1], (BLK, 128)) for s in range(CAP)], axis=0
            )
            ask = jnp.concatenate([ask] * (length // 128), axis=1)
            chooser = jnp.where(
                (ask == (sj // BLK).astype(F32)) & (si % BLK == sj % BLK), 1.0, 0.0
            ).astype(BF)
            sent = mm(chooser, tkv[...]).astype(BF)
            blk_out[d - 1, 0:slot_rows] = sent[:, 0:cols]
            blk_out[d - 1, slot_rows : 2 * slot_rows] = sent[:, cols : 2 * cols]
            block_copy(d).start()

    for d in range(1, kvn):

        @pl.when(me >= d)
        def _():
            coarse_copy(d).wait_recv()

    coarse_k = coarse[:, 0:nb].reshape(kvn * nb, cols)
    coarse_vt = coarse[:, nb : 2 * nb].reshape(kvn * nb, cols).T
    ck = [coarse_k[:, k * HEAD : (k + 1) * HEAD].astype(BF) for k in range(kv_dev)]
    cvt = [coarse_vt[k * HEAD : (k + 1) * HEAD].astype(BF) for k in range(kv_dev)]
    wide = per_kv * n
    dk = iota((n, wide), 0)
    dq = iota((n, wide), 1) % n
    near_bias = jnp.where((dk // BLK == dq // BLK) & (dk <= dq), 0.0, NEG)
    cr = iota((kvn * nb, wide), 0)
    cb = (me - cr // nb) * nb + cr % nb
    lane = iota((kvn * nb, wide), 1) % n
    for c in range(tpn):
        pos = me * length + c * n + lane
        seen = (cb >= 0) & ((cb + 1) * BLK - 1 <= pos)
        for k in range(kv_dev):
            sc = jnp.where(seen, mm(ck[k], qp[c, k]), NEG)
            near_k = tkv[c * n : (c + 1) * n, k * HEAD : (k + 1) * HEAD]
            sn = mm(near_k, qt[c, k]) + near_bias
            peak = jnp.max(sc, axis=0, keepdims=True)
            top = jnp.max(sn, axis=0, keepdims=True)
            pw = jnp.where(seen, jnp.exp(sc - peak), 0.0)
            pn = jnp.exp(sn - top)
            weight = pw / jnp.maximum(jnp.sum(pw, axis=0, keepdims=True), 1.0)
            part_c[c, k] = gt[c, k : k + 1] * mm(cvt[k], weight.astype(BF))
            part_n[c, k] = mm(vt[k * HEAD : (k + 1) * HEAD, c * n : (c + 1) * n], pn.astype(BF))
            part_m[c, k : k + 1] = top
            part_l[c, k : k + 1] = jnp.sum(pn, axis=0, keepdims=True)

    for d in range(1, kvn):

        @pl.when(me >= d)
        def _():
            block_copy(d).wait_recv()

    far = (kvn - 1) * slot_rows
    far_k = blks[:, 0:slot_rows].reshape(far, cols)
    far_vt = blks[:, slot_rows : 2 * slot_rows].reshape(far, cols).astype(F32).T.astype(BF)
    kr = [far_k[:, k * HEAD : (k + 1) * HEAD] for k in range(kv_dev)]
    vr = [far_vt[k * HEAD : (k + 1) * HEAD] for k in range(kv_dev)]

    def attend(chunk):
        here = pl.ds(pl.multiple_of(chunk * n, n), n)
        far_bias = jnp.concatenate(
            [
                jnp.broadcast_to(maskb[d * 8 + s : d * 8 + s + 1, here], (BLK, n))
                for d in range(1, kvn)
                for s in range(CAP)
            ],
            axis=0,
        )
        far_bias = jnp.concatenate([far_bias] * per_kv, axis=1)
        mixed = []
        for k in range(kv_dev):
            sf = mm(kr[k], qt[chunk, k]) + far_bias
            top_near = part_m[chunk, k : k + 1]
            top = jnp.maximum(jnp.max(sf, axis=0, keepdims=True), top_near)
            shrink = jnp.exp(top_near - top)
            pf = jnp.exp(sf - top)
            norm = jnp.sum(pf, axis=0, keepdims=True) + part_l[chunk, k : k + 1] * shrink
            fine = mm(vr[k], pf.astype(BF)) + part_n[chunk, k] * shrink
            g_fine = gt[chunk, kv_dev + k : kv_dev + k + 1]
            both = part_c[chunk, k] + fine * (g_fine / norm)
            mixed += [both[:, g * n : (g + 1) * n] for g in range(per_kv)]
        return jnp.concatenate(mixed, axis=0).T.astype(BF)

    mix_out[...] = attend(tpn - 1 - tp)
    mix_copy.start()
    mix_own[...] = attend(tp)
    loads[8].wait()
    step = 512
    for c in range(0, width, step):
        acc[:, c : c + step] = mm(mix_own[...], wo[:, c : c + step])
    loads[9].wait()
    weight_copy.wait_recv()
    mix_copy.wait_recv()
    square = jnp.zeros((n, 1), F32)
    for c in range(0, width, step):
        part = acc[:, c : c + step] + mm(mix_in[...], wo2[:, c : c + step])
        acc[:, c : c + step] = part
        square = square + jnp.sum(part * part, axis=1, keepdims=True)
    factor = lax.rsqrt(square * (1.0 / width) + EPS)
    pieces = 4
    span = n // pieces
    stores = []
    for i in range(pieces):
        rows = slice(i * span, (i + 1) * span)
        acc[rows] = acc[rows] * factor[rows] * gain[...]
        store = pltpu.make_async_copy(acc.at[pl.ds(i * span, span)], out_h.at[0, pl.ds(i * span, span)], osem.at[i])
        store.start()
        stores.append(store)
    for store in stores:
        store.wait()
    weight_copy.wait_send()
    mix_copy.wait_send()
    for d in range(1, kvn):

        @pl.when(me >= d)
        def _():
            req_copy(d).wait_send()

        @pl.when(me + d < kvn)
        def _():
            coarse_copy(d).wait_send()
            block_copy(d).wait_send()


def on_device(kvn, tpn, tokens, wq, wk, wv, wg, cw, wo, gain, chosen):
    length, width = tokens.shape[1:]
    cols = wk.shape[1]
    qcols = wq.shape[1]
    table = jnp.asarray(rope_table(kvn, length))
    nb = length // BLK
    rows_out = length // tpn
    kv_dev = cols // HEAD
    wide = (qcols // cols) * rows_out
    V = pltpu.VMEM
    dma = pltpu.SemaphoreType.DMA
    scratch = [
        V((length, width), BF),
        V((width, 2 * cols), BF),
        V((width, qcols), BF),
        V((wg.shape[1], width), BF),
        V(cw.shape, F32),
        V(wo.shape, BF),
        V(wo.shape, BF),
        V((1, width), F32),
        V(chosen.shape[1:], jnp.int32),
        V(table.shape[1:], F32),
        V((kvn, 8, 128), F32),
        V((kvn, 8, 128), F32),
        V((kvn * 8, length), F32),
        V((length, 2 * cols), BF),
        V((cols, length), BF),
        V((kvn, 2 * nb, cols), F32),
        V((kvn - 1, 2 * CAP * BLK, cols), BF),
        V((kvn - 1, 2 * CAP * BLK, cols), BF),
        V((tpn, kv_dev, HEAD, wide), BF),
        V((tpn, kv_dev, HEAD, wide), BF),
        V((tpn, 2 * kv_dev, wide), F32),
        V((tpn, kv_dev, HEAD, wide), F32),
        V((tpn, kv_dev, HEAD, wide), F32),
        V((tpn, kv_dev, wide), F32),
        V((tpn, kv_dev, wide), F32),
        V((rows_out, qcols), BF),
        V((rows_out, qcols), BF),
        V((rows_out, qcols), BF),
        V((rows_out, width), F32),
        dma((10,)),
        dma((4,)),
        dma((kvn,)),
        dma((kvn,)),
        dma((kvn,)),
        dma((kvn,)),
        dma((kvn,)),
        dma((kvn,)),
        dma,
        dma,
        dma,
        dma,
    ]
    return pl.pallas_call(
        functools.partial(kernel, kvn, tpn),
        out_shape=jax.ShapeDtypeStruct((1, rows_out, width), F32),
        in_specs=[ANY] * 10,
        out_specs=ANY,
        scratch_shapes=scratch,
        compiler_params=pltpu.CompilerParams(
            collective_id=0, has_side_effects=True, vmem_limit_bytes=67043328
        ),
    )(tokens, wq, wk, wv, wg.T, cw, wo, gain.reshape(1, width), chosen, table)


def solution(mesh):
    in_specs = (
        P("dp", "kv", None),
        P(None, "tp"),
        P(None, "tp"),
        P(None, "tp"),
        P(),
        P(),
        P("tp", None),
        P(),
        P("dp", "kv", None),
    )
    return jax.shard_map(
        functools.partial(on_device, mesh.shape["kv"], mesh.shape["tp"]),
        mesh=mesh,
        in_specs=in_specs,
        out_specs=P("dp", ("kv", "tp"), None),
        check_vma=False,
    )
```

```python
import functools

import numpy as np
import jax
import jax.numpy as jnp
from jax import lax
from jax.experimental import pallas as pl
from jax.experimental.pallas import tpu as pltpu
from jax.sharding import PartitionSpec as P

HEAD = 64
BLK = 32
CAP = 2
NEG = -1e30
ROPE_BASE = 500000.0
EPS = 1e-06
F32 = jnp.float32
BF = jnp.bfloat16
ANY = pl.BlockSpec(memory_space=pl.ANY)


def mm(a, b):
    return jnp.dot(a, b, preferred_element_type=F32)


def mm_t(a, b):
    return lax.dot_general(a, b, (((1,), (1,)), ((), ())), preferred_element_type=F32)


def iota(shape, dim):
    return lax.broadcasted_iota(jnp.int32, shape, dim)


def rope_table(kvn, length):
    half = HEAD // 2
    inverse = ROPE_BASE ** (-np.arange(half) * (2.0 / HEAD))
    angles = np.arange(kvn * length)[None, :] * inverse[:, None]
    table = np.stack([np.cos(angles), np.sin(angles)]).astype(np.float32)
    return table.reshape(2, half, kvn, length).transpose(2, 0, 1, 3).copy()


def kernel(
    kvn,
    tpn,
    tok_h,
    wq_h,
    wk_h,
    wv_h,
    wg_h,
    cw_h,
    wo_h,
    gain_h,
    chosen_h,
    tab_h,
    acc,
    tok,
    wkv,
    wq,
    wg,
    cw,
    wo,
    wo2,
    gain,
    chosen,
    tab,
    reqs,
    reqin,
    maskb,
    tkv,
    vt,
    coarse,
    blk_out,
    blks,
    qp,
    qt,
    gt,
    part_c,
    part_n,
    part_m,
    part_l,
    mix_own,
    mix_out,
    mix_in,
    lsem,
    req_s,
    req_r,
    co_s,
    co_r,
    bl_s,
    bl_r,
    wo_s,
    wo_r,
    mx_s,
    mx_r,
):
    dp = lax.axis_index("dp")
    me = lax.axis_index("kv")
    tp = lax.axis_index("tp")
    length, width = tok.shape
    cols = wkv.shape[1] // 2
    kv_dev = cols // HEAD
    heads = wq.shape[1] // HEAD
    per_kv = heads // kv_dev
    nb = length // BLK
    total_blocks = kvn * nb
    rows_out = length // tpn
    slot_rows = CAP * BLK

    def local(src, dst, index):
        return pltpu.make_async_copy(src, dst, lsem.at[index])

    loads = [
        local(chosen_h.at[0], chosen, 0),
        local(tab_h.at[me], tab, 1),
        local(tok_h.at[0], tok, 2),
        local(wk_h, wkv.at[:, 0:cols], 3),
        local(wv_h, wkv.at[:, cols : 2 * cols], 4),
        local(cw_h, cw, 5),
        local(wq_h, wq, 6),
        local(wg_h, wg, 7),
        local(wo_h, wo, 8),
        local(gain_h, gain, 9),
    ]
    for load in loads:
        load.start()

    barrier = pltpu.get_barrier_semaphore()
    for d in range(1, kvn):
        peer = lax.rem(me + d, kvn)
        pl.semaphore_signal(
            barrier, inc=1, device_id=(dp, peer, tp), device_id_type=pl.DeviceIdType.MESH
        )
    other = (dp, me, tpn - 1 - tp)
    pl.semaphore_signal(barrier, inc=1, device_id=other, device_id_type=pl.DeviceIdType.MESH)

    def remote(src, dst, send, recv, target):
        return pltpu.make_async_remote_copy(
            src_ref=src,
            dst_ref=dst,
            send_sem=send,
            recv_sem=recv,
            device_id=target,
            device_id_type=pl.DeviceIdType.MESH,
        )

    def req_copy(d):
        return remote(
            reqs.at[d], reqin.at[d], req_s.at[d], req_r.at[d], (dp, lax.rem(me - d + kvn, kvn), tp)
        )

    def coarse_copy(d):
        return remote(
            coarse.at[0], coarse.at[d], co_s.at[d], co_r.at[d], (dp, lax.rem(me + d, kvn), tp)
        )

    def block_copy(d):
        return remote(
            blk_out.at[d - 1],
            blks.at[d - 1],
            bl_s.at[d],
            bl_r.at[d],
            (dp, lax.rem(me + d, kvn), tp),
        )

    weight_copy = remote(wo_h, wo2, wo_s, wo_r, other)
    mix_copy = remote(mix_out, mix_in, mx_s, mx_r, other)

    for d in range(1, kvn):

        @pl.when(me < d)
        def _():
            blks[d - 1] = jnp.zeros(blks.shape[1:], BF)
            coarse[d] = jnp.zeros(coarse.shape[1:], F32)

    loads[0].wait()
    listed = chosen[...]
    lane_blk = iota((nb, total_blocks), 1)
    hit = jnp.zeros((nb, total_blocks), F32)
    for t in range(listed.shape[1]):
        hit = jnp.where(listed[:, t : t + 1] == lane_blk, 1.0, hit)
    needed = jnp.max(hit, axis=0, keepdims=True)
    gi = iota((total_blocks, total_blocks), 0)
    gj = iota((total_blocks, total_blocks), 1)
    before = jnp.where((gi // nb == gj // nb) & (gi < gj), 1.0, 0.0).astype(BF)
    rank = mm(jnp.broadcast_to(needed, (8, total_blocks)).astype(BF), before)[0:1]
    ra = iota((kvn * 8, total_blocks), 0)
    ja = iota((kvn * 8, total_blocks), 1)
    pick = jnp.where(
        (needed > 0.5)
        & (rank == (ra % 8).astype(F32))
        & (ra % 8 < CAP)
        & (ja // nb == me - ra // 8),
        1.0,
        0.0,
    )
    wanted = jnp.sum(pick * ((ja % nb) + 1).astype(F32), axis=1, keepdims=True) - 1.0
    reqs[...] = jnp.broadcast_to(wanted, (kvn * 8, 128)).reshape(kvn, 8, 128)

    @pl.when(me > 0)
    def _():
        pl.semaphore_wait(barrier, kvn)

    for d in range(1, kvn):

        @pl.when(me >= d)
        def _():
            req_copy(d).start()

    loads[1].wait()
    cos_t = tab[0]
    sin_t = tab[1]
    cos_n = jnp.concatenate([cos_t, cos_t] * kv_dev, axis=0).T
    sin_n = jnp.concatenate([-sin_t, sin_t] * kv_dev, axis=0).T

    for index in (2, 3, 4, 5):
        loads[index].wait()
    both = mm(tok[...], wkv[...]).astype(BF)
    tkv[:, cols : 2 * cols] = both[:, cols : 2 * cols]
    both = both.astype(F32)
    key_f = both[:, 0:cols]
    val_f = both[:, cols : 2 * cols]

    def compress(x, index):
        weight = jnp.concatenate([cw[index]] * kv_dev, axis=1)
        packed = jnp.sum(x.reshape(nb, BLK, cols) * weight[None], axis=1)
        return packed.astype(BF).astype(F32)

    coarse[0, 0:nb] = compress(key_f, 0)
    coarse[0, nb : 2 * nb] = compress(val_f, 1)
    half = HEAD // 2
    low = iota((length, cols), 1) % HEAD < half
    swapped = jnp.where(low, pltpu.roll(key_f, cols - half, 1), pltpu.roll(key_f, half, 1))
    tkv[:, 0:cols] = (key_f * cos_n + swapped * sin_n).astype(BF)

    vt[...] = val_f.T.astype(BF)

    @pl.when(me == 0)
    def _():
        pl.semaphore_wait(barrier, kvn)

    for d in range(1, kvn):

        @pl.when(me + d < kvn)
        def _():
            coarse_copy(d).start()

    spread = jnp.where(iota((nb, length), 1) // BLK == iota((nb, length), 0), 1.0, 0.0)
    member = mm(mm_t(pick, hit), spread)
    maskb[...] = jnp.where(member > 0.5, 0.0, NEG)


    loads[6].wait()
    n = rows_out
    scale = HEAD ** (-0.5)
    query_t = mm(tok[...], wq[...]).astype(BF).astype(F32).T * scale
    loads[7].wait()
    gates = jax.nn.sigmoid(mm_t(wg[...], tok[...]))
    for h in range(heads):
        k, g = h // per_kv, h % per_kv
        first = query_t[h * HEAD : h * HEAD + half]
        second = query_t[h * HEAD + half : (h + 1) * HEAD]
        plain = query_t[h * HEAD : (h + 1) * HEAD].astype(BF)
        turned_low = (first * cos_t - second * sin_t).astype(BF)
        turned_high = (second * cos_t + first * sin_t).astype(BF)
        for c in range(tpn):
            lanes = slice(g * n, (g + 1) * n)
            here = slice(c * n, (c + 1) * n)
            qp[c, k, :, lanes] = plain[:, here]
            qt[c, k, 0:half, lanes] = turned_low[:, here]
            qt[c, k, half:HEAD, lanes] = turned_high[:, here]
            for branch in range(2):
                gate = jnp.zeros((1, n), F32)
                for t in range(tpn):
                    row = (branch * tpn + t) * heads + h
                    gate = jnp.where(tp == t, gates[row : row + 1, here], gate)
                gt[c, branch * kv_dev + k : branch * kv_dev + k + 1, lanes] = gate

    wide = per_kv * n
    dk = iota((n, wide), 0)
    dq = iota((n, wide), 1) % n
    near_bias = jnp.where((dk // BLK == dq // BLK) & (dk <= dq), 0.0, NEG)
    for c in range(tpn):
        for k in range(kv_dev):
            near_k = tkv[c * n : (c + 1) * n, k * HEAD : (k + 1) * HEAD]
            sn = mm(near_k, qt[c, k]) + near_bias
            top = jnp.max(sn, axis=0, keepdims=True)
            pn = jnp.exp(sn - top)
            part_n[c, k] = mm(vt[k * HEAD : (k + 1) * HEAD, c * n : (c + 1) * n], pn.astype(BF))
            part_m[c, k : k + 1] = top
            part_l[c, k : k + 1] = jnp.sum(pn, axis=0, keepdims=True)

    si = iota((slot_rows, length), 0)
    sj = iota((slot_rows, length), 1)
    for d in range(1, kvn):

        @pl.when(me + d < kvn)
        def _():
            req_copy(d).wait_recv()
            tile = reqin[d]
            ask = jnp.concatenate(
                [jnp.broadcast_to(tile[s : s + 1], (BLK, 128)) for s in range(CAP)], axis=0
            )
            ask = jnp.concatenate([ask] * (length // 128), axis=1)
            chooser = jnp.where(
                (ask == (sj // BLK).astype(F32)) & (si % BLK == sj % BLK), 1.0, 0.0
            ).astype(BF)
            sent = mm(chooser, tkv[...]).astype(BF)
            blk_out[d - 1, 0:slot_rows] = sent[:, 0:cols]
            blk_out[d - 1, slot_rows : 2 * slot_rows] = sent[:, cols : 2 * cols]
            block_copy(d).start()

    for d in range(1, kvn):

        @pl.when(me >= d)
        def _():
            coarse_copy(d).wait_recv()

    weight_copy.start()
    coarse_k = coarse[:, 0:nb].reshape(kvn * nb, cols)
    coarse_vt = coarse[:, nb : 2 * nb].reshape(kvn * nb, cols).T
    ck = [coarse_k[:, k * HEAD : (k + 1) * HEAD].astype(BF) for k in range(kv_dev)]
    cvt = [coarse_vt[k * HEAD : (k + 1) * HEAD].astype(BF) for k in range(kv_dev)]
    cr = iota((kvn * nb, wide), 0)
    cb = (me - cr // nb) * nb + cr % nb
    lane = iota((kvn * nb, wide), 1) % n
    for c in range(tpn):
        pos = me * length + c * n + lane
        seen = (cb >= 0) & ((cb + 1) * BLK - 1 <= pos)
        for k in range(kv_dev):
            sc = jnp.where(seen, mm(ck[k], qp[c, k]), NEG)
            peak = jnp.max(sc, axis=0, keepdims=True)
            pw = jnp.where(seen, jnp.exp(sc - peak), 0.0)
            weight = pw / jnp.maximum(jnp.sum(pw, axis=0, keepdims=True), 1.0)
            part_c[c, k] = gt[c, k : k + 1] * mm(cvt[k], weight.astype(BF))

    for d in range(1, kvn):

        @pl.when(me >= d)
        def _():
            block_copy(d).wait_recv()

    far = (kvn - 1) * slot_rows
    far_k = blks[:, 0:slot_rows].reshape(far, cols)
    far_vt = blks[:, slot_rows : 2 * slot_rows].reshape(far, cols).astype(F32).T.astype(BF)
    kr = [far_k[:, k * HEAD : (k + 1) * HEAD] for k in range(kv_dev)]
    vr = [far_vt[k * HEAD : (k + 1) * HEAD] for k in range(kv_dev)]

    def attend(chunk):
        here = pl.ds(pl.multiple_of(chunk * n, n), n)
        far_bias = jnp.concatenate(
            [
                jnp.broadcast_to(maskb[d * 8 + s : d * 8 + s + 1, here], (BLK, n))
                for d in range(1, kvn)
                for s in range(CAP)
            ],
            axis=0,
        )
        far_bias = jnp.concatenate([far_bias] * per_kv, axis=1)
        mixed = []
        for k in range(kv_dev):
            sf = mm(kr[k], qt[chunk, k]) + far_bias
            top_near = part_m[chunk, k : k + 1]
            top = jnp.maximum(jnp.max(sf, axis=0, keepdims=True), top_near)
            shrink = jnp.exp(top_near - top)
            pf = jnp.exp(sf - top)
            norm = jnp.sum(pf, axis=0, keepdims=True) + part_l[chunk, k : k + 1] * shrink
            fine = mm(vr[k], pf.astype(BF)) + part_n[chunk, k] * shrink
            g_fine = gt[chunk, kv_dev + k : kv_dev + k + 1]
            both = part_c[chunk, k] + fine * (g_fine / norm)
            mixed += [both[:, g * n : (g + 1) * n] for g in range(per_kv)]
        return jnp.concatenate(mixed, axis=0).T.astype(BF)

    mix_out[...] = attend(tpn - 1 - tp)
    mix_copy.start()
    mix_own[...] = attend(tp)
    loads[8].wait()
    step = 512
    for c in range(0, width, step):
        acc[0, :, c : c + step] = mm(mix_own[...], wo[:, c : c + step])
    loads[9].wait()
    weight_copy.wait_recv()
    mix_copy.wait_recv()
    square = jnp.zeros((n, 1), F32)
    for c in range(0, width, step):
        part = acc[0, :, c : c + step] + mm(mix_in[...], wo2[:, c : c + step])
        acc[0, :, c : c + step] = part
        square = square + jnp.sum(part * part, axis=1, keepdims=True)
    factor = lax.rsqrt(square * (1.0 / width) + EPS)
    for c in range(0, width, step):
        acc[0, :, c : c + step] = acc[0, :, c : c + step] * factor * gain[:, c : c + step]
    weight_copy.wait_send()
    mix_copy.wait_send()
    for d in range(1, kvn):

        @pl.when(me >= d)
        def _():
            req_copy(d).wait_send()

        @pl.when(me + d < kvn)
        def _():
            coarse_copy(d).wait_send()
            block_copy(d).wait_send()


def on_device(kvn, tpn, tokens, wq, wk, wv, wg, cw, wo, gain, chosen):
    length, width = tokens.shape[1:]
    cols = wk.shape[1]
    qcols = wq.shape[1]
    table = jnp.asarray(rope_table(kvn, length))
    nb = length // BLK
    rows_out = length // tpn
    kv_dev = cols // HEAD
    wide = (qcols // cols) * rows_out
    V = pltpu.VMEM
    dma = pltpu.SemaphoreType.DMA
    scratch = [
        V((length, width), BF),
        V((width, 2 * cols), BF),
        V((width, qcols), BF),
        V((wg.shape[1], width), BF),
        V(cw.shape, F32),
        V(wo.shape, BF),
        V(wo.shape, BF),
        V((1, width), F32),
        V(chosen.shape[1:], jnp.int32),
        V(table.shape[1:], F32),
        V((kvn, 8, 128), F32),
        V((kvn, 8, 128), F32),
        V((kvn * 8, length), F32),
        V((length, 2 * cols), BF),
        V((cols, length), BF),
        V((kvn, 2 * nb, cols), F32),
        V((kvn - 1, 2 * CAP * BLK, cols), BF),
        V((kvn - 1, 2 * CAP * BLK, cols), BF),
        V((tpn, kv_dev, HEAD, wide), BF),
        V((tpn, kv_dev, HEAD, wide), BF),
        V((tpn, 2 * kv_dev, wide), F32),
        V((tpn, kv_dev, HEAD, wide), F32),
        V((tpn, kv_dev, HEAD, wide), F32),
        V((tpn, kv_dev, wide), F32),
        V((tpn, kv_dev, wide), F32),
        V((rows_out, qcols), BF),
        V((rows_out, qcols), BF),
        V((rows_out, qcols), BF),
        dma((10,)),
        dma((kvn,)),
        dma((kvn,)),
        dma((kvn,)),
        dma((kvn,)),
        dma((kvn,)),
        dma((kvn,)),
        dma,
        dma,
        dma,
        dma,
    ]
    return pl.pallas_call(
        functools.partial(kernel, kvn, tpn),
        out_shape=pltpu.VMEM((1, rows_out, width), F32),
        in_specs=[ANY] * 10,
        out_specs=pl.BlockSpec(memory_space=pltpu.VMEM),
        scratch_shapes=scratch,
        compiler_params=pltpu.CompilerParams(
            collective_id=0, has_side_effects=True, vmem_limit_bytes=60000000
        ),
    )(tokens, wq, wk, wv, wg.T, cw, wo, gain.reshape(1, width), chosen, table)


def solution(mesh):
    in_specs = (
        P("dp", "kv", None),
        P(None, "tp"),
        P(None, "tp"),
        P(None, "tp"),
        P(),
        P(),
        P("tp", None),
        P(),
        P("dp", "kv", None),
    )
    return jax.shard_map(
        functools.partial(on_device, mesh.shape["kv"], mesh.shape["tp"]),
        mesh=mesh,
        in_specs=in_specs,
        out_specs=P("dp", ("kv", "tp"), None),
        check_vma=False,
    )
```

```python
import functools

import numpy as np
import jax
import jax.numpy as jnp
from jax import lax
from jax.experimental import pallas as pl
from jax.experimental.pallas import tpu as pltpu
from jax.sharding import PartitionSpec as P

HEAD = 64
BLK = 32
CAP = 2
NEG = -1e30
ROPE_BASE = 500000.0
EPS = 1e-06
F32 = jnp.float32
BF = jnp.bfloat16
ANY = pl.BlockSpec(memory_space=pl.ANY)


def mm(a, b):
    return jnp.dot(a, b, preferred_element_type=F32)


def mm_t(a, b):
    return lax.dot_general(a, b, (((1,), (1,)), ((), ())), preferred_element_type=F32)


def iota(shape, dim):
    return lax.broadcasted_iota(jnp.int32, shape, dim)


def rope_table(kvn, length):
    half = HEAD // 2
    inverse = ROPE_BASE ** (-np.arange(half) * (2.0 / HEAD))
    angles = np.arange(kvn * length)[None, :] * inverse[:, None]
    table = np.stack([np.cos(angles), np.sin(angles)]).astype(np.float32)
    return table.reshape(2, half, kvn, length).transpose(2, 0, 1, 3).copy()


def kernel(
    kvn,
    tpn,
    tok_h,
    wq_h,
    wk_h,
    wv_h,
    wg_h,
    cw_h,
    wo_h,
    gain_h,
    chosen_h,
    tab_h,
    acc,
    tok,
    wkv,
    wq,
    wg,
    cw,
    wo,
    wo2,
    gain,
    chosen,
    tab,
    reqs,
    reqin,
    maskb,
    tkv,
    vt,
    coarse,
    blk_out,
    blks,
    qp,
    qt,
    gt,
    part_c,
    part_n,
    part_m,
    part_l,
    mix_own,
    mix_out,
    mix_in,
    lsem,
    req_s,
    req_r,
    co_s,
    co_r,
    bl_s,
    bl_r,
    wo_s,
    wo_r,
    mx_s,
    mx_r,
):
    dp = lax.axis_index("dp")
    me = lax.axis_index("kv")
    tp = lax.axis_index("tp")
    length, width = tok.shape
    cols = wkv.shape[1] // 2
    kv_dev = cols // HEAD
    heads = wq.shape[1] // HEAD
    per_kv = heads // kv_dev
    nb = length // BLK
    total_blocks = kvn * nb
    rows_out = length // tpn
    slot_rows = CAP * BLK

    def local(src, dst, index):
        return pltpu.make_async_copy(src, dst, lsem.at[index])

    loads = [
        local(chosen_h.at[0], chosen, 0),
        local(tab_h.at[me], tab, 1),
        local(tok_h.at[0], tok, 2),
        local(wk_h, wkv.at[:, 0:cols], 3),
        local(wv_h, wkv.at[:, cols : 2 * cols], 4),
        local(cw_h, cw, 5),
        local(wq_h, wq, 6),
        local(wg_h, wg, 7),
        local(wo_h, wo, 8),
        local(gain_h, gain, 9),
    ]
    for load in loads:
        load.start()

    barrier = pltpu.get_barrier_semaphore()
    for d in range(1, kvn):
        peer = lax.rem(me + d, kvn)
        pl.semaphore_signal(
            barrier, inc=1, device_id=(dp, peer, tp), device_id_type=pl.DeviceIdType.MESH
        )
    other = (dp, me, tpn - 1 - tp)
    pl.semaphore_signal(barrier, inc=1, device_id=other, device_id_type=pl.DeviceIdType.MESH)

    def remote(src, dst, send, recv, target):
        return pltpu.make_async_remote_copy(
            src_ref=src,
            dst_ref=dst,
            send_sem=send,
            recv_sem=recv,
            device_id=target,
            device_id_type=pl.DeviceIdType.MESH,
        )

    def req_copy(d):
        return remote(
            reqs.at[d], reqin.at[d], req_s.at[d], req_r.at[d], (dp, lax.rem(me - d + kvn, kvn), tp)
        )

    def coarse_copy(d):
        return remote(
            coarse.at[0], coarse.at[d], co_s.at[d], co_r.at[d], (dp, lax.rem(me + d, kvn), tp)
        )

    def block_copy(d):
        return remote(
            blk_out.at[d - 1],
            blks.at[d - 1],
            bl_s.at[d],
            bl_r.at[d],
            (dp, lax.rem(me + d, kvn), tp),
        )

    weight_copy = remote(wo_h, wo2, wo_s, wo_r, other)
    mix_copy = remote(mix_out, mix_in, mx_s, mx_r, other)

    for d in range(1, kvn):

        @pl.when(me < d)
        def _():
            blks[d - 1] = jnp.zeros(blks.shape[1:], BF)
            coarse[d] = jnp.zeros(coarse.shape[1:], F32)

    def publish():
        for d in range(1, kvn):

            @pl.when(me + d < kvn)
            def _():
                coarse_copy(d).start()

        weight_copy.start()

    loads[0].wait()
    listed = chosen[...]
    lane_blk = iota((nb, total_blocks), 1)
    hit = jnp.zeros((nb, total_blocks), F32)
    for t in range(listed.shape[1]):
        hit = jnp.where(listed[:, t : t + 1] == lane_blk, 1.0, hit)
    needed = jnp.max(hit, axis=0, keepdims=True)
    gi = iota((total_blocks, total_blocks), 0)
    gj = iota((total_blocks, total_blocks), 1)
    before = jnp.where((gi // nb == gj // nb) & (gi < gj), 1.0, 0.0).astype(BF)
    rank = mm(jnp.broadcast_to(needed, (8, total_blocks)).astype(BF), before)[0:1]
    ra = iota((kvn * 8, total_blocks), 0)
    ja = iota((kvn * 8, total_blocks), 1)
    pick = jnp.where(
        (needed > 0.5)
        & (rank == (ra % 8).astype(F32))
        & (ra % 8 < CAP)
        & (ja // nb == me - ra // 8),
        1.0,
        0.0,
    )
    wanted = jnp.sum(pick * ((ja % nb) + 1).astype(F32), axis=1, keepdims=True) - 1.0
    reqs[...] = jnp.broadcast_to(wanted, (kvn * 8, 128)).reshape(kvn, 8, 128)

    @pl.when(me > 0)
    def _():
        pl.semaphore_wait(barrier, kvn)

    for d in range(1, kvn):

        @pl.when(me >= d)
        def _():
            req_copy(d).start()

    loads[1].wait()
    cos_t = tab[0]
    sin_t = tab[1]
    cos_n = jnp.concatenate([cos_t, cos_t] * kv_dev, axis=0).T
    sin_n = jnp.concatenate([-sin_t, sin_t] * kv_dev, axis=0).T

    for index in (2, 3, 4, 5):
        loads[index].wait()
    both = mm(tok[...], wkv[...]).astype(BF)
    tkv[:, cols : 2 * cols] = both[:, cols : 2 * cols]
    both = both.astype(F32)
    key_f = both[:, 0:cols]
    val_f = both[:, cols : 2 * cols]

    def compress(x, index):
        weight = jnp.concatenate([cw[index]] * kv_dev, axis=1)
        packed = jnp.sum(x.reshape(nb, BLK, cols) * weight[None], axis=1)
        return packed.astype(BF).astype(F32)

    coarse[0, 0:nb] = compress(key_f, 0)
    coarse[0, nb : 2 * nb] = compress(val_f, 1)
    half = HEAD // 2
    low = iota((length, cols), 1) % HEAD < half
    swapped = jnp.where(low, pltpu.roll(key_f, cols - half, 1), pltpu.roll(key_f, half, 1))
    tkv[:, 0:cols] = (key_f * cos_n + swapped * sin_n).astype(BF)

    vt[...] = val_f.T.astype(BF)

    @pl.when(me > 0)
    def _():
        publish()

    spread = jnp.where(iota((nb, length), 1) // BLK == iota((nb, length), 0), 1.0, 0.0)
    member = mm(mm_t(pick, hit), spread)
    maskb[...] = jnp.where(member > 0.5, 0.0, NEG)


    loads[6].wait()
    n = rows_out
    scale = HEAD ** (-0.5)
    query_t = mm(tok[...], wq[...]).astype(BF).astype(F32).T * scale
    for h in range(heads):
        k, g = h // per_kv, h % per_kv
        first = query_t[h * HEAD : h * HEAD + half]
        second = query_t[h * HEAD + half : (h + 1) * HEAD]
        plain = query_t[h * HEAD : (h + 1) * HEAD].astype(BF)
        turned_low = (first * cos_t - second * sin_t).astype(BF)
        turned_high = (second * cos_t + first * sin_t).astype(BF)
        for c in range(tpn):
            lanes = slice(g * n, (g + 1) * n)
            here = slice(c * n, (c + 1) * n)
            qp[c, k, :, lanes] = plain[:, here]
            qt[c, k, 0:half, lanes] = turned_low[:, here]
            qt[c, k, half:HEAD, lanes] = turned_high[:, here]

    @pl.when(me == 0)
    def _():
        pl.semaphore_wait(barrier, kvn)
        publish()

    si = iota((slot_rows, length), 0)
    sj = iota((slot_rows, length), 1)

    def serve(d):
        req_copy(d).wait_recv()
        tile = reqin[d]
        ask = jnp.concatenate(
            [jnp.broadcast_to(tile[s : s + 1], (BLK, 128)) for s in range(CAP)], axis=0
        )
        ask = jnp.concatenate([ask] * (length // 128), axis=1)
        chooser = jnp.where(
            (ask == (sj // BLK).astype(F32)) & (si % BLK == sj % BLK), 1.0, 0.0
        ).astype(BF)
        sent = mm(chooser, tkv[...]).astype(BF)
        blk_out[d - 1, 0:slot_rows] = sent[:, 0:cols]
        blk_out[d - 1, slot_rows : 2 * slot_rows] = sent[:, cols : 2 * cols]
        block_copy(d).start()

    for d in reversed(range(1, kvn)):

        @pl.when((me > 0) & (me + d < kvn))
        def _():
            serve(d)

    loads[7].wait()
    gates = jax.nn.sigmoid(mm_t(wg[...], tok[...]))
    for h in range(heads):
        k, g = h // per_kv, h % per_kv
        for c in range(tpn):
            lanes = slice(g * n, (g + 1) * n)
            here = slice(c * n, (c + 1) * n)
            for branch in range(2):
                gate = jnp.zeros((1, n), F32)
                for t in range(tpn):
                    row = (branch * tpn + t) * heads + h
                    gate = jnp.where(tp == t, gates[row : row + 1, here], gate)
                gt[c, branch * kv_dev + k : branch * kv_dev + k + 1, lanes] = gate

    wide = per_kv * n
    dk = iota((n, wide), 0)
    dq = iota((n, wide), 1) % n
    near_bias = jnp.where((dk // BLK == dq // BLK) & (dk <= dq), 0.0, NEG)
    for c in range(tpn):
        for k in range(kv_dev):
            near_k = tkv[c * n : (c + 1) * n, k * HEAD : (k + 1) * HEAD]
            sn = mm(near_k, qt[c, k]) + near_bias
            top = jnp.max(sn, axis=0, keepdims=True)
            pn = jnp.exp(sn - top)
            part_n[c, k] = mm(vt[k * HEAD : (k + 1) * HEAD, c * n : (c + 1) * n], pn.astype(BF))
            part_m[c, k : k + 1] = top
            part_l[c, k : k + 1] = jnp.sum(pn, axis=0, keepdims=True)

    for d in range(1, kvn - 1):

        @pl.when((me == 0) & (me + d < kvn))
        def _():
            serve(d)

    for d in range(1, kvn):

        @pl.when(me >= d)
        def _():
            coarse_copy(d).wait_recv()

    coarse_k = coarse[:, 0:nb].reshape(kvn * nb, cols)
    coarse_vt = coarse[:, nb : 2 * nb].reshape(kvn * nb, cols).T
    ck = [coarse_k[:, k * HEAD : (k + 1) * HEAD].astype(BF) for k in range(kv_dev)]
    cvt = [coarse_vt[k * HEAD : (k + 1) * HEAD].astype(BF) for k in range(kv_dev)]
    cr = iota((kvn * nb, wide), 0)
    cb = (me - cr // nb) * nb + cr % nb
    lane = iota((kvn * nb, wide), 1) % n
    for c in range(tpn):
        pos = me * length + c * n + lane
        seen = (cb >= 0) & ((cb + 1) * BLK - 1 <= pos)
        for k in range(kv_dev):
            sc = jnp.where(seen, mm(ck[k], qp[c, k]), NEG)
            peak = jnp.max(sc, axis=0, keepdims=True)
            pw = jnp.where(seen, jnp.exp(sc - peak), 0.0)
            weight = pw / jnp.maximum(jnp.sum(pw, axis=0, keepdims=True), 1.0)
            part_c[c, k] = gt[c, k : k + 1] * mm(cvt[k], weight.astype(BF))

    @pl.when((me == 0) & (kvn > 1))
    def _():
        serve(kvn - 1)

    for d in range(1, kvn):

        @pl.when(me >= d)
        def _():
            block_copy(d).wait_recv()

    far = (kvn - 1) * slot_rows
    far_k = blks[:, 0:slot_rows].reshape(far, cols)
    far_vt = blks[:, slot_rows : 2 * slot_rows].reshape(far, cols).astype(F32).T.astype(BF)
    kr = [far_k[:, k * HEAD : (k + 1) * HEAD] for k in range(kv_dev)]
    vr = [far_vt[k * HEAD : (k + 1) * HEAD] for k in range(kv_dev)]

    def attend(chunk):
        here = pl.ds(pl.multiple_of(chunk * n, n), n)
        far_bias = jnp.concatenate(
            [
                jnp.broadcast_to(maskb[d * 8 + s : d * 8 + s + 1, here], (BLK, n))
                for d in range(1, kvn)
                for s in range(CAP)
            ],
            axis=0,
        )
        far_bias = jnp.concatenate([far_bias] * per_kv, axis=1)
        mixed = []
        for k in range(kv_dev):
            sf = mm(kr[k], qt[chunk, k]) + far_bias
            top_near = part_m[chunk, k : k + 1]
            top = jnp.maximum(jnp.max(sf, axis=0, keepdims=True), top_near)
            shrink = jnp.exp(top_near - top)
            pf = jnp.exp(sf - top)
            norm = jnp.sum(pf, axis=0, keepdims=True) + part_l[chunk, k : k + 1] * shrink
            fine = mm(vr[k], pf.astype(BF)) + part_n[chunk, k] * shrink
            g_fine = gt[chunk, kv_dev + k : kv_dev + k + 1]
            both = part_c[chunk, k] + fine * (g_fine / norm)
            mixed += [both[:, g * n : (g + 1) * n] for g in range(per_kv)]
        return jnp.concatenate(mixed, axis=0).T.astype(BF)

    mix_out[...] = attend(tpn - 1 - tp)
    mix_copy.start()
    mix_own[...] = attend(tp)
    loads[8].wait()
    step = 512
    for c in range(0, width, step):
        acc[0, :, c : c + step] = mm(mix_own[...], wo[:, c : c + step])
    loads[9].wait()
    weight_copy.wait_recv()
    mix_copy.wait_recv()
    square = jnp.zeros((n, 1), F32)
    for c in range(0, width, step):
        part = acc[0, :, c : c + step] + mm(mix_in[...], wo2[:, c : c + step])
        acc[0, :, c : c + step] = part
        square = square + jnp.sum(part * part, axis=1, keepdims=True)
    factor = lax.rsqrt(square * (1.0 / width) + EPS)
    for c in range(0, width, step):
        acc[0, :, c : c + step] = acc[0, :, c : c + step] * factor * gain[:, c : c + step]
    weight_copy.wait_send()
    mix_copy.wait_send()
    for d in range(1, kvn):

        @pl.when(me >= d)
        def _():
            req_copy(d).wait_send()

        @pl.when(me + d < kvn)
        def _():
            coarse_copy(d).wait_send()
            block_copy(d).wait_send()


def on_device(kvn, tpn, tokens, wq, wk, wv, wg, cw, wo, gain, chosen):
    length, width = tokens.shape[1:]
    cols = wk.shape[1]
    qcols = wq.shape[1]
    table = jnp.asarray(rope_table(kvn, length))
    nb = length // BLK
    rows_out = length // tpn
    kv_dev = cols // HEAD
    wide = (qcols // cols) * rows_out
    V = pltpu.VMEM
    dma = pltpu.SemaphoreType.DMA
    scratch = [
        V((length, width), BF),
        V((width, 2 * cols), BF),
        V((width, qcols), BF),
        V((wg.shape[1], width), BF),
        V(cw.shape, F32),
        V(wo.shape, BF),
        V(wo.shape, BF),
        V((1, width), F32),
        V(chosen.shape[1:], jnp.int32),
        V(table.shape[1:], F32),
        V((kvn, 8, 128), F32),
        V((kvn, 8, 128), F32),
        V((kvn * 8, length), F32),
        V((length, 2 * cols), BF),
        V((cols, length), BF),
        V((kvn, 2 * nb, cols), F32),
        V((kvn - 1, 2 * CAP * BLK, cols), BF),
        V((kvn - 1, 2 * CAP * BLK, cols), BF),
        V((tpn, kv_dev, HEAD, wide), BF),
        V((tpn, kv_dev, HEAD, wide), BF),
        V((tpn, 2 * kv_dev, wide), F32),
        V((tpn, kv_dev, HEAD, wide), F32),
        V((tpn, kv_dev, HEAD, wide), F32),
        V((tpn, kv_dev, wide), F32),
        V((tpn, kv_dev, wide), F32),
        V((rows_out, qcols), BF),
        V((rows_out, qcols), BF),
        V((rows_out, qcols), BF),
        dma((10,)),
        dma((kvn,)),
        dma((kvn,)),
        dma((kvn,)),
        dma((kvn,)),
        dma((kvn,)),
        dma((kvn,)),
        dma,
        dma,
        dma,
        dma,
    ]
    return pl.pallas_call(
        functools.partial(kernel, kvn, tpn),
        out_shape=pltpu.VMEM((1, rows_out, width), F32),
        in_specs=[ANY] * 10,
        out_specs=pl.BlockSpec(memory_space=pltpu.VMEM),
        scratch_shapes=scratch,
        compiler_params=pltpu.CompilerParams(
            collective_id=0, has_side_effects=True, vmem_limit_bytes=60000000
        ),
    )(tokens, wq, wk, wv, wg.T, cw, wo, gain.reshape(1, width), chosen, table)


def solution(mesh):
    in_specs = (
        P("dp", "kv", None),
        P(None, "tp"),
        P(None, "tp"),
        P(None, "tp"),
        P(),
        P(),
        P("tp", None),
        P(),
        P("dp", "kv", None),
    )
    return jax.shard_map(
        functools.partial(on_device, mesh.shape["kv"], mesh.shape["tp"]),
        mesh=mesh,
        in_specs=in_specs,
        out_specs=P("dp", ("kv", "tp"), None),
        check_vma=False,
    )
```
